256 devices in a mesh: grp: 2 (over y), sp: 32 (over z, core), tp: 4 (over x).
Axes of the slice: x: 4, y: 2, z: 16, core: 2. Of those that a mesh axis runs over, the one named last changes fastest.
The devices are a block of a 4x16x16 slice.
Arguments:
- ssm_input: bfloat16 [8192, 1024], P(('grp', 'sp'), 'tp'), parts along dimension 0, may hold values from -6 to 6
- residual_in: bfloat16 [8192, 2048], P(('grp', 'sp')), parts along dimension 0, may hold values from -4 to 4
- log_step: float32 [64], P('tp'), may hold values from -6.91 to -2.3
- decay_real: float32 [64, 64], P('tp'), may hold values from -34 to 0, as said below
- freq: float32 [64, 64], P('tp'), may hold values from 0.5 to 8
- in_real: float32 [64, 64, 16], P('tp'), may hold values from -1 to 1
- in_imag: float32 [64, 64, 16], P('tp'), may hold values from -1 to 1
- out_real: float32 [64, 16, 64], P('tp'), may hold values from -0.5 to 0.5
- out_imag: float32 [64, 16, 64], P('tp'), may hold values from -0.5 to 0.5
- skip: float32 [1024], P('tp'), may hold values from -3 to 3
- w_glu: bfloat16 [1024, 1024], replicated, may hold values from -0.1875 to 0.1875
- b_glu: float32 [1024], replicated, may hold values from -3 to 3
- w_branch: bfloat16 [1024, 2048], replicated, may hold values from -0.1875 to 0.1875
- norm_gain: float32 [2048], replicated, may hold values from 0.1 to 1.9
- w_gate: bfloat16 [2048, 5632], P('sp', 'tp'), may hold values from -0.125 to 0.125
- w_up: bfloat16 [2048, 5632], P('sp', 'tp'), may hold values from -0.125 to 0.125
- w_down: bfloat16 [5632, 2048], P('tp', 'sp'), may hold values from -0.078125 to 0.078125
Outputs:
- mixed: bfloat16 [8192, 2048], P(('grp', 'sp', 'tp')), parts along dimension 0
The draws below stay inside these ranges and needn't reach their ends.
There are 2 independent parts, one for each index of `grp`. The reference program is written for one: setup_inputs(seed, part) draws one part's arguments, and reference() takes and returns one part's arrays. A program takes and returns all parts, laid end to end along the dimension named above; an argument that names none is the same for every part. Nothing has to cross between parts.
Inputs may be any that keep to these rules, and one draw needn't show every extreme that they name: `decay_real`: negative in every entry.
All inputs are finite; a program needn't handle non-finite values.
Results may differ from the reference program's by a relative error of at most 0.015.
Values may be sent and summed in bfloat16 or wider, within the bound.
A program may use at most 128 MiB of HBM per device.

```python
import math
import jax
import jax.numpy as jnp
from jax import lax

D = 2048
FF = 5632
SSM_GROUPS = 64
SSM_GROUP = 16
SSM_STATE = 64
TOK_DEV = 128
SSM_WIDTH = 1024
TOKENS = 4096
N_SP = 32


def decay_plan(key):
    subkeys = jax.random.split(jax.random.fold_in(key, 11), 5)
    fast_share = 0.5
    fast_group = jax.random.uniform(subkeys[0], (SSM_GROUPS,), jnp.float32) < fast_share
    slow_rate = jax.random.uniform(subkeys[1], (SSM_GROUPS,), jnp.float32, 0.3, 2.0) / TOKENS
    fast_rate = jax.random.uniform(subkeys[2], (SSM_GROUPS,), jnp.float32, 1.0 / 100.0, 1.0 / 30.0)
    decay_rate = jnp.where(fast_group, fast_rate, slow_rate)
    log_steps = jax.random.uniform(subkeys[3], (SSM_GROUPS,), jnp.float32, math.log(0.001), math.log(0.1))
    spread = jax.random.uniform(subkeys[4], (SSM_GROUPS, SSM_STATE), jnp.float32, 0.5, 1.0)
    return (log_steps, decay_rate, spread)


def draw_log_step(key, part):
    return decay_plan(key)[0]


def draw_decay_real(key, part):
    log_steps, decay_rate, spread = decay_plan(key)
    return -decay_rate[:, None] * spread / jnp.exp(log_steps)[:, None]


def shard_levels(rng, shape, pieces, smallest, largest):
    gain = 1.0
    for position, blocks in pieces:
        heights = jax.random.uniform(jax.random.fold_in(jax.random.fold_in(rng, 6), position), (blocks,), jnp.float32, smallest / len(pieces), largest / len(pieces))
        gain = gain * jnp.repeat(jnp.exp(heights), shape[position] // blocks).reshape((-1,) + (1,) * (len(shape) - 1 - position))
    return gain


def centred(own_key, shape, scale, most, cuts=(), kind=jnp.bfloat16):
    result = scale * jax.random.normal(own_key, shape, jnp.float32)
    if cuts:
        result = result * shard_levels(own_key, shape, cuts, -0.22, 0.18)
    return jnp.clip(result, -most, most).astype(kind)


def setup_inputs(seed: int = 0, part: int = 0) -> dict:
    key_of = jax.random.split(jax.random.key(seed), 18)
    own_keys = jax.random.split(jax.random.fold_in(key_of[17], part), 18)
    return {
        "ssm_input": centred(own_keys[0], (TOKENS, SSM_WIDTH), 1.0, 6.0, ((0, 32), (1, 4))),
        "residual_in": centred(own_keys[1], (TOKENS, D), 0.5, 4.0, ((0, 32),)),
        "log_step": draw_log_step(jax.random.fold_in(key_of[17], 71), part),
        "decay_real": draw_decay_real(jax.random.fold_in(key_of[17], 71), part),
        "freq": jnp.clip(0.5 + 7.5 * jax.random.uniform(key_of[4], (SSM_GROUPS, SSM_STATE), jnp.float32) ** shard_levels(key_of[4], (SSM_GROUPS, SSM_STATE), ((0, 4),), -0.2, 0.2), 0.5, 8.0),
        "in_real": centred(key_of[5], (SSM_GROUPS, SSM_STATE, SSM_GROUP), (2 * SSM_GROUP) ** -0.5, 1.0, ((0, 4),), jnp.float32),
        "in_imag": centred(key_of[6], (SSM_GROUPS, SSM_STATE, SSM_GROUP), (2 * SSM_GROUP) ** -0.5, 1.0, ((0, 4),), jnp.float32),
        "out_real": centred(key_of[7], (SSM_GROUPS, SSM_GROUP, SSM_STATE), (2 * SSM_STATE) ** -0.5, 0.5, ((0, 4),), jnp.float32),
        "out_imag": centred(key_of[8], (SSM_GROUPS, SSM_GROUP, SSM_STATE), (2 * SSM_STATE) ** -0.5, 0.5, ((0, 4),), jnp.float32),
        "skip": centred(key_of[9], (SSM_WIDTH,), 0.5, 3.0, ((0, 4),), jnp.float32),
        "w_glu": centred(key_of[10], (SSM_WIDTH, SSM_WIDTH), SSM_WIDTH ** -0.5, 0.1875),
        "b_glu": centred(key_of[11], (SSM_WIDTH,), 0.5, 3.0, (), jnp.float32),
        "w_branch": centred(key_of[12], (SSM_WIDTH, D), SSM_WIDTH ** -0.5, 0.1875),
        "norm_gain": jnp.clip(1.0 + 0.18 * jax.random.normal(key_of[13], (D,), jnp.float32), 0.1, 1.9),
        "w_gate": centred(key_of[14], (D, FF), D ** -0.5, 0.125, ((0, 32), (1, 4))),
        "w_up": centred(key_of[15], (D, FF), D ** -0.5, 0.125, ((0, 32), (1, 4))),
        "w_down": centred(key_of[16], (FF, D), FF ** -0.5, 0.078125, ((0, 4), (1, 32))),
    }


EPS = 1e-06

def discretize(log_step, decay_real, freq, in_real, in_imag):
    step_size = jnp.exp(log_step)[:, None]
    magnitude = jnp.exp(decay_real * step_size)
    abar_re = magnitude * jnp.cos(freq * step_size)
    abar_im = magnitude * jnp.sin(freq * step_size)
    denominator = decay_real * decay_real + freq * freq
    less_re = abar_re - 1.0
    less_im = abar_im
    hold_re = ((less_re * decay_real + less_im * freq) / denominator)[..., None]
    hold_im = ((less_im * decay_real - less_re * freq) / denominator)[..., None]
    bbar_re = hold_re * in_real - hold_im * in_imag
    bbar_im = hold_re * in_imag + hold_im * in_real
    return (step_size, abar_re, abar_im, bbar_re, bbar_im)

def powers(decay_real, freq, step_size, length):
    steps_up = (jnp.arange(length, dtype=jnp.int32) + 1).astype(jnp.float32)[:, None, None]
    magnitude = jnp.exp((decay_real * step_size)[None] * steps_up)
    phase = (freq * step_size)[None] * steps_up
    return (magnitude * jnp.cos(phase), magnitude * jnp.sin(phase))

def compose(earlier, later):
    a1r, a1i, b1r, b1i = earlier
    a2r, a2i, b2r, b2i = later
    return (a2r * a1r - a2i * a1i, a2r * a1i + a2i * a1r, a2r * b1r - a2i * b1i + b2r, a2r * b1i + a2i * b1r + b2i)

def local_states(inputs, abar_re, abar_im, bbar_re, bbar_im):
    hp = lax.Precision.HIGHEST
    drive_re = jnp.einsum('lgm,gpm->lgp', inputs, bbar_re, precision=hp)
    drive_im = jnp.einsum('lgm,gpm->lgp', inputs, bbar_im, precision=hp)
    full_re = jnp.broadcast_to(abar_re[None], drive_re.shape)
    full_im = jnp.broadcast_to(abar_im[None], drive_re.shape)
    scanned = lax.associative_scan(compose, (full_re, full_im, drive_re, drive_im), axis=0)
    return (scanned[2], scanned[3])

def readout(state_re, state_im, out_real, out_imag, skip_mat, inputs):
    hp = lax.Precision.HIGHEST
    values = jnp.einsum('lgp,gmp->lgm', state_re, out_real, precision=hp) - jnp.einsum('lgp,gmp->lgm', state_im, out_imag, precision=hp) + skip_mat[None] * inputs
    values = jax.nn.gelu(values)
    return values.reshape(values.shape[0], -1).astype(jnp.bfloat16)

def reference(ssm_input, residual_in, log_step, decay_real, freq, in_real, in_imag, out_real, out_imag, skip, w_glu, b_glu, w_branch, norm_gain, w_gate, w_up, w_down):
    step_size, abar_re, abar_im, bbar_re, bbar_im = discretize(log_step, decay_real, freq, in_real, in_imag)
    pow_re, pow_im = powers(decay_real, freq, step_size, TOK_DEV)
    skip_mat = skip.reshape(SSM_GROUPS, SSM_GROUP)
    blocks = ssm_input.astype(jnp.float32).reshape(N_SP, TOK_DEV, SSM_GROUPS, SSM_GROUP)

    def one_block(carried, inputs):
        local_re, local_im = local_states(inputs, abar_re, abar_im, bbar_re, bbar_im)
        state_re = local_re + pow_re * carried[0][None] - pow_im * carried[1][None]
        state_im = local_im + pow_re * carried[1][None] + pow_im * carried[0][None]
        mixer_out = readout(state_re, state_im, out_real, out_imag, skip_mat, inputs)
        return ((state_re[-1], state_im[-1]), mixer_out)
    start_state = (jnp.zeros((SSM_GROUPS, SSM_STATE), jnp.float32), jnp.zeros((SSM_GROUPS, SSM_STATE), jnp.float32))
    unused, outputs = lax.scan(one_block, start_state, blocks)
    mixer_out = outputs.reshape(TOKENS, SSM_WIDTH)
    glu_pre = jnp.dot(mixer_out, w_glu, preferred_element_type=jnp.float32) + b_glu
    gated = (mixer_out.astype(jnp.float32) * jax.nn.sigmoid(glu_pre)).astype(jnp.bfloat16)
    stream = residual_in.astype(jnp.float32) + jnp.dot(gated, w_branch, preferred_element_type=jnp.float32)
    scale_rows = lax.rsqrt(lax.optimization_barrier(jnp.mean(stream * stream, axis=-1, keepdims=True)) + EPS)
    normed = (stream * scale_rows * norm_gain).astype(jnp.bfloat16)
    gate_sum = jnp.dot(normed, w_gate, preferred_element_type=jnp.float32)
    up_sum = jnp.dot(normed, w_up, preferred_element_type=jnp.float32)
    hidden = (jax.nn.silu(gate_sum) * up_sum).astype(jnp.bfloat16)
    return (stream + jnp.dot(hidden, w_down, preferred_element_type=jnp.float32)).astype(jnp.bfloat16)
```

```python
import functools

import jax
import jax.numpy as jnp
from jax import lax
from jax.experimental import pallas as pl
from jax.experimental.pallas import tpu as pltpu
from jax.sharding import Mesh
from jax.sharding import PartitionSpec as P

SP = ("sp_0", "sp_1")
GRP_SP = ("grp", "sp_0", "sp_1")
GRP_SP_TP = ("grp", "sp_0", "sp_1", "tp")
EPS = 1e-06
LANES = 128
SPAN = 16
ROWS8 = 8
BF = jnp.bfloat16
F32 = jnp.float32
MESH = pl.DeviceIdType.MESH


def mod(a, n):
    return lax.rem(a + 8 * n, n)


def cmul(ar, ai, br, bi):
    return ar * br - ai * bi, ar * bi + ai * br


def dot(a, b):
    return jnp.dot(a, b, preferred_element_type=F32)


def dot_t(a, b):
    return lax.dot_general(a, b, (((1,), (1,)), ((), ())), preferred_element_type=F32)


def tile(v, k):
    return v[:, k * LANES : (k + 1) * LANES]


def swap_halves(v, forward):
    rows, width = v.shape
    half = width // LANES // 2
    low = lax.broadcasted_iota(jnp.int32, (rows, LANES), 1) < LANES // 2
    first, second = [], []
    for k in range(half):
        one, two = (tile(v, 2 * k), tile(v, 2 * k + 1)) if forward else (tile(v, k), tile(v, half + k))
        first.append(jnp.where(low, one, pltpu.roll(two, LANES // 2, 1)))
        second.append(jnp.where(low, pltpu.roll(one, LANES // 2, 1), two))
    if forward:
        return jnp.concatenate(first + second, axis=1)
    return jnp.concatenate([t for pair in zip(first, second) for t in pair], axis=1)


def kernel(
    dims,
    u_ref, ls_ref, dr_ref, fq_ref, inr_ref, ini_ref, our_ref, oui_ref, skip_ref, bglu_ref, gain_ref,
    resid_hbm, wglu_hbm, wbr_hbm, wg_hbm, wu_hbm, wd_hbm,
    out_ref,
    wglu, wbr, resid, w, tab_b, tab_c, drive, states, est, gst, mo, mrecv, act, stream, own, part, sbuf, rbuf,
    cp_sem, st_send, st_recv, e_send, e_recv, g_send, g_recv, m_send, m_recv,
    xf_send, xf_recv, xh_send, xh_recv, p_send, p_recv, ag_send, ag_recv, rs_send, rs_recv,
):
    n_z, n_x, tiles, slots = dims
    quads = n_z // n_x
    z, c, x = lax.axis_index("sp_0"), lax.axis_index("sp_1"), lax.axis_index("tp")
    zq = lax.div(z, n_x)
    right, left = {"sp_0": mod(z + 1, n_z)}, {"sp_0": mod(z - 1, n_z)}
    other = {"sp_1": 1 - c}
    tok, width = u_ref.shape
    groups, lanes_state = dr_ref.shape
    n_state = groups * lanes_state
    half_z = n_z // 2
    own_rows, d = stream.shape
    d_half = d // 2
    d_block = d_half // n_z
    ff_pad = slots * LANES

    barrier = pltpu.get_barrier_semaphore()

    def greet(k, unused):
        pl.semaphore_signal(barrier, inc=1, device_id={"sp_0": mod(z + k, n_z)}, device_id_type=MESH)
        return unused

    lax.fori_loop(1, n_z, greet, 0)
    for k in range(1, n_x):
        pl.semaphore_signal(barrier, inc=1, device_id={"tp": mod(x + k, n_x)}, device_id_type=MESH)
    pl.semaphore_signal(barrier, inc=1, device_id=other, device_id_type=MESH)

    local = [
        pltpu.make_async_copy(wglu_hbm, wglu, cp_sem.at[0]),
        pltpu.make_async_copy(wbr_hbm, wbr, cp_sem.at[1]),
        pltpu.make_async_copy(resid_hbm.at[pl.ds(pl.multiple_of(x * own_rows, own_rows), own_rows)], resid, cp_sem.at[2]),
    ]
    for copy in local:
        copy.start()

    diag = lax.broadcasted_iota(jnp.int32, (groups, groups), 0) == lax.broadcasted_iota(jnp.int32, (groups, groups), 1)
    step = jnp.sum(jnp.where(diag, jnp.broadcast_to(jnp.exp(ls_ref[...]), (groups, groups)), 0.0), axis=1, keepdims=True)
    dr, fq = dr_ref[...], fq_ref[...]
    mag = jnp.exp(dr * step)
    abar_re, abar_im = mag * jnp.cos(fq * step), mag * jnp.sin(fq * step)
    denominator = dr * dr + fq * fq
    less_re = abar_re - 1.0
    hold_re = (less_re * dr + abar_im * fq) / denominator
    hold_im = (abar_im * dr - less_re * fq) / denominator

    def row_form(v):
        twice = jnp.concatenate([v, v], axis=1)
        row = lax.broadcasted_iota(jnp.int32, (groups, LANES), 0)
        lane = lax.broadcasted_iota(jnp.int32, (groups, LANES), 1)
        pieces = []
        for k in range(n_state // LANES):
            keep = row == 2 * k + lax.div(lane, lanes_state)
            pieces.append(jnp.sum(jnp.where(keep, twice, 0.0), axis=0, keepdims=True))
        return jnp.concatenate(pieces, axis=1)

    a_re, a_im = row_form(abar_re), row_form(abar_im)
    h_re, h_im = row_form(hold_re), row_form(hold_im)

    group_size = width // groups
    pair_rows = 2 * group_size
    row = lax.broadcasted_iota(jnp.int32, (pair_rows, LANES), 0)
    lane = lax.broadcasted_iota(jnp.int32, (pair_rows, LANES), 1)
    keep = lax.div(row, group_size) == lax.div(lane, lanes_state)

    tab_b[...] = jnp.zeros_like(tab_b)
    tab_c[...] = jnp.zeros_like(tab_c)

    def put(table, k, col, value):
        table[k * pair_rows : (k + 1) * pair_rows, col + k * LANES : col + (k + 1) * LANES] = jnp.where(keep, value, 0.0).astype(BF)

    def twice_of(ref, k):
        v = ref[k * pair_rows : (k + 1) * pair_rows, :]
        return jnp.concatenate([v, v], axis=1)

    for k in range(n_state // LANES):
        hr, hi = tile(h_re, k), tile(h_im, k)
        ir, ii = twice_of(inr_ref, k), twice_of(ini_ref, k)
        put(tab_b, k, 0, hr * ir - hi * ii)
        put(tab_b, k, n_state, hr * ii + hi * ir)
        put(tab_c, k, 0, twice_of(our_ref, k))
        put(tab_c, k, n_state, -twice_of(oui_ref, k))

    to_row = lax.broadcasted_iota(jnp.int32, (tok, tok), 0)
    to_col = lax.broadcasted_iota(jnp.int32, (tok, tok), 1)
    order = (to_col == lax.rem(to_row, ROWS8) * SPAN + lax.div(to_row, ROWS8)).astype(F32).astype(BF)
    back = (to_row == lax.rem(to_col, ROWS8) * SPAN + lax.div(to_col, ROWS8)).astype(F32).astype(BF)
    u_perm = dot(order, u_ref[...])
    drive[...] = dot(u_perm.astype(BF), tab_b[...])

    ar, ai = jnp.broadcast_to(a_re, (ROWS8, n_state)), jnp.broadcast_to(a_im, (ROWS8, n_state))
    s_re = drive[0:ROWS8, 0:n_state]
    s_im = drive[0:ROWS8, n_state:]
    for j in range(1, SPAN):
        at = slice(j * ROWS8, (j + 1) * ROWS8)
        p_re, p_im = cmul(ar, ai, s_re, s_im)
        s_re = p_re + drive[at, 0:n_state]
        s_im = p_im + drive[at, n_state:]
        drive[at, 0:n_state] = s_re
        drive[at, n_state:] = s_im

    pw = [(ar, ai)]
    for _ in range(8):
        pw.append(cmul(*pw[-1], *pw[-1]))
    chunk = lax.broadcasted_iota(jnp.int32, (ROWS8, n_state), 0)

    def shifted(v, by):
        return jnp.where(chunk >= by, pltpu.roll(v, by, 0), 0.0)

    i_re, i_im = s_re, s_im
    for level, by in ((4, 1), (5, 2), (6, 4)):
        q_re, q_im = cmul(*pw[level], shifted(i_re, by), shifted(i_im, by))
        i_re, i_im = i_re + q_re, i_im + q_im
    before_re, before_im = shifted(i_re, 1), shifted(i_im, 1)
    end_re, end_im = i_re[ROWS8 - 1 :, :], i_im[ROWS8 - 1 :, :]
    est[0, 0:1, :] = end_re
    est[0, 1:2, :] = end_im
    a128 = (pw[7][0][0:1], pw[7][1][0:1])
    a256 = (pw[8][0][0:1], pw[8][1][0:1])

    for s in range(slots):
        if s * quads + quads - 1 >= tiles:

            @pl.when(s * quads + zq >= tiles)
            def _():
                for m in range(3):
                    at = (m * slots + s) * LANES
                    w[:, :, at : at + LANES] = jnp.zeros((2, d_half, LANES), BF)

    pl.semaphore_wait(barrier, n_z - 1 + n_x - 1 + 1)

    e_copy = pltpu.make_async_remote_copy(
        src_ref=est.at[0], dst_ref=est.at[1], send_sem=e_send.at[0], recv_sem=e_recv.at[0], device_id=other, device_id_type=MESH
    )
    e_copy.start()
    e_copy.wait_recv()
    oth_re, oth_im = est[1, 0:1, :], est[1, 1:2, :]
    first = c == 0
    e0_re, e0_im = jnp.where(first, end_re, oth_re), jnp.where(first, end_im, oth_im)
    e1_re, e1_im = jnp.where(first, oth_re, end_re), jnp.where(first, oth_im, end_im)
    g_re, g_im = cmul(*a128, e0_re, e0_im)
    est[2, 0:1, :] = g_re + e1_re
    est[2, 1:2, :] = g_im + e1_im

    def g_copy(to):
        return pltpu.make_async_remote_copy(
            src_ref=est.at[2], dst_ref=gst.at[z], send_sem=g_send.at[to], recv_sem=g_recv.at[z],
            device_id={"sp_0": to}, device_id_type=MESH,
        )

    def g_start(to, unused):
        g_copy(to).start()
        return unused

    lax.fori_loop(z + 1, n_z, g_start, 0)

    sources = (wg_hbm, wu_hbm, wd_hbm)

    def w_at(core, rows, m, s):
        return w.at[core, rows, pl.ds(pl.multiple_of((m * slots + s) * LANES, LANES), LANES)]

    z_rows = pl.ds(pl.multiple_of(z * d_block, d_block), d_block)
    all_rows = pl.ds(0, d_half)

    def st_place(j):
        s = lax.div(j, quads)
        return s, lax.rem(j, quads) * n_x + mod(x - s, n_x)

    def st_copy(m, j, s, to):
        src = sources[m].at[:, pl.ds(pl.multiple_of(j * LANES, LANES), LANES)]
        return pltpu.make_async_remote_copy(
            src_ref=src, dst_ref=w_at(c, z_rows, m, s), send_sem=st_send.at[m, j], recv_sem=st_recv.at[m],
            device_id={"sp_0": to}, device_id_type=MESH,
        )

    for m in range(3):

        def st_start(j, unused, m=m):
            s, to = st_place(j)

            @pl.when(to != z)
            def _():
                st_copy(m, j, s, to).start()

            @pl.when(to == z)
            def _():
                src = sources[m].at[:, pl.ds(pl.multiple_of(j * LANES, LANES), LANES)]
                pltpu.make_async_copy(src, w_at(c, z_rows, m, s), st_recv.at[m]).start()

            return unused

        lax.fori_loop(0, tiles, st_start, 0)

    def add_state(frm, carry):
        g_got = pltpu.make_async_remote_copy(
            src_ref=est.at[2], dst_ref=gst.at[frm], send_sem=g_send.at[frm], recv_sem=g_recv.at[frm],
            device_id={"sp_0": frm}, device_id_type=MESH,
        )
        g_got.wait_recv()
        n_re, n_im = cmul(*a256, *carry)
        return n_re + gst[frm, 0:1, :], n_im + gst[frm, 1:2, :]

    zero_row = jnp.zeros((1, n_state), F32)
    in_re, in_im = lax.fori_loop(0, z, add_state, (zero_row, zero_row))
    t_re, t_im = cmul(*a128, in_re, in_im)
    in_re, in_im = jnp.where(first, in_re, t_re + oth_re), jnp.where(first, in_im, t_im + oth_im)

    one, nil = jnp.ones((ROWS8, n_state), F32), jnp.zeros((ROWS8, n_state), F32)
    r_re, r_im = one, nil
    for level, bit in ((4, 1), (5, 2), (6, 4)):
        has = lax.rem(lax.div(chunk, bit), 2) == 1
        r_re, r_im = cmul(r_re, r_im, jnp.where(has, pw[level][0], one), jnp.where(has, pw[level][1], nil))
    c_re, c_im = cmul(r_re, r_im, jnp.broadcast_to(in_re, (ROWS8, n_state)), jnp.broadcast_to(in_im, (ROWS8, n_state)))
    c_re, c_im = c_re + before_re, c_im + before_im
    for jj in range(SPAN // 2):
        out_re, out_im = [], []
        for j in (2 * jj, 2 * jj + 1):
            at = slice(j * ROWS8, (j + 1) * ROWS8)
            c_re, c_im = cmul(ar, ai, c_re, c_im)
            out_re.append(drive[at, 0:n_state] + c_re)
            out_im.append(drive[at, n_state:] + c_im)
        at = slice(2 * jj * ROWS8, 2 * (jj + 1) * ROWS8)
        states[at, 0:n_state] = jnp.concatenate(out_re, axis=0).astype(BF)
        states[at, n_state:] = jnp.concatenate(out_im, axis=0).astype(BF)
    values = dot_t(states[...], tab_c[...]) + skip_ref[...] * u_perm
    cubic = 0.7978845608028654 * (values + 0.044715 * (values * values * values))
    values = values * (0.5 * (1.0 + jnp.tanh(cubic)))
    mixed = dot(back, values.astype(BF)).astype(BF)
    for k in range(n_x):
        mo[k] = mixed[k * own_rows : (k + 1) * own_rows, :]

    def m_copy(k):
        to = mod(x + k, n_x)
        return pltpu.make_async_remote_copy(
            src_ref=mo.at[to], dst_ref=mrecv.at[x], send_sem=m_send.at[k], recv_sem=m_recv.at[k],
            device_id={"tp": to}, device_id_type=MESH,
        )

    for k in range(1, n_x):
        m_copy(k).start()
    mrecv[x] = mo[x]
    for copy in local:
        copy.wait()
    for k in range(1, n_x):
        m_copy(k).wait_recv()
    rows_in = jnp.concatenate([mrecv[k] for k in range(n_x)], axis=1)
    glu = dot(rows_in, wglu[...]) + bglu_ref[...]
    gated = (rows_in.astype(F32) / (1.0 + jnp.exp(-glu))).astype(BF)
    st = resid[...].astype(F32) + dot(gated, wbr[...])
    stream[...] = st
    scale = lax.rsqrt(jnp.mean(st * st, axis=-1, keepdims=True) + EPS)
    act[z] = swap_halves(st * scale * gain_ref[...], True).astype(BF)

    half_rows = own_rows // 2

    def ag_copy(way, k):
        to, block = (right, mod(z - k + 1, n_z)) if way == 0 else (left, mod(z + k - 1, n_z))
        ref = act.at[block] if k < half_z else act.at[block, pl.ds(way * half_rows, half_rows)]
        return pltpu.make_async_remote_copy(
            src_ref=ref, dst_ref=ref, send_sem=ag_send.at[way, k - 1], recv_sem=ag_recv.at[way, k - 1],
            device_id=to, device_id_type=MESH,
        )

    def ag_got(way, k):
        block = mod(z - k, n_z) if way == 0 else mod(z + k, n_z)
        ref = act.at[block] if k < half_z else act.at[block, pl.ds(way * half_rows, half_rows)]
        return pltpu.make_async_remote_copy(
            src_ref=ref, dst_ref=ref, send_sem=ag_send.at[way, k - 1], recv_sem=ag_recv.at[way, k - 1],
            device_id=right, device_id_type=MESH,
        )

    def ag_start(k):
        for way in range(2):
            ag_copy(way, k).start()

    def ag_next(k):
        for way in range(2):
            ag_got(way, k).wait_recv()
            if k < half_z:
                ag_copy(way, k + 1).start()

    def role(r):
        s = mod(x - z - r, n_x)
        return s, s * quads + zq < tiles

    x_to = {0: {"tp": mod(x + 1, n_x)}, 1: {"tp": mod(x - 1, n_x)}}
    mid = d_half // 2
    halves = (pl.ds(0, mid), pl.ds(mid, mid))

    def remote(ref, send, recv, to):
        return pltpu.make_async_remote_copy(
            src_ref=ref, dst_ref=ref, send_sem=send, recv_sem=recv, device_id=to, device_id_type=MESH
        )

    def xf_copy(m, way, s):
        return remote(w_at(c, all_rows, m, s), xf_send.at[m, way], xf_recv.at[m, way], x_to[way])

    def xh_copy(m, way, s):
        return remote(w_at(c, halves[way], m, s), xh_send.at[m, way], xh_recv.at[m, way], x_to[way])

    def p_copy(m, r, s):
        return remote(w_at(c, all_rows, m, s), p_send.at[m, r], p_recv.at[m, r], other)

    def x_owner(m):
        s, valid = role(0)

        @pl.when(valid)
        def _():
            remote(w_at(c, all_rows, m, s), st_send.at[m, 0], st_recv.at[m], right).wait_recv()
            xf_copy(m, 0, s).start()
            xf_copy(m, 1, s).start()
            p_copy(m, 0, s).start()

    def x_relay(m):
        for way, r in ((0, 1), (1, 3)):
            s, valid = role(r)

            @pl.when(valid)
            def _(way=way, r=r, s=s):
                xf_copy(m, way, s).wait_recv()
                xh_copy(m, way, s).start()
                p_copy(m, r, s).start()

    def x_last(m):
        s, valid = role(2)

        @pl.when(valid)
        def _():
            for way in range(2):
                xh_copy(m, way, s).wait_recv()
            p_copy(m, 2, s).start()

    def x_partner(m):
        for r in range(4):
            s, valid = role(r)

            @pl.when(valid)
            def _(r=r, s=s):
                remote(w_at(1 - c, all_rows, m, s), p_send.at[m, r], p_recv.at[m, r], other).wait_recv()

    meanwhile = [
        lambda: x_owner(0), lambda: x_owner(1),
        lambda: x_relay(0), lambda: x_owner(2), lambda: x_relay(1), lambda: x_last(0),
        lambda: x_relay(2), lambda: x_last(1), lambda: x_last(2),
        lambda: [x_partner(m) for m in range(3)],
    ]
    places = {1: (0, 1), 2: (2,), 3: (3, 4), 4: (5,), 5: (6, 7), 6: (), 7: (8,)}
    done = set()
    ag_start(1)
    for k in range(1, half_z + 1):
        ag_next(k)
        for at in places.get(k, ()):
            meanwhile[at]()
            done.add(at)
    for at in range(len(meanwhile)):
        if at not in done:
            meanwhile[at]()

    rbuf[0, 0, half_rows:, :] = jnp.zeros((own_rows - half_rows, d), BF)
    rbuf[1, 0, 0:half_rows, :] = jnp.zeros((half_rows, d), BF)

    def rs_copy(way, i, whole):
        rows = pl.ds(0, own_rows) if whole else pl.ds(way * half_rows, half_rows)
        return pltpu.make_async_remote_copy(
            src_ref=sbuf.at[way, i, rows], dst_ref=rbuf.at[way, i, rows],
            send_sem=rs_send.at[way, i], recv_sem=rs_recv.at[way, i],
            device_id=right if way == 0 else left, device_id_type=MESH,
        )

    def ring_step(i, unused):
        far = half_z - i
        one_at = mod(z + far, n_z)
        two_at = jnp.where(i == 0, z, mod(z - far, n_z))
        rows2 = jnp.concatenate([act[one_at], act[two_at]], axis=0)
        sums = dot(rows2[:, 0:d_half], w[0, :, 0 : 2 * ff_pad]) + dot(rows2[:, d_half:], w[1, :, 0 : 2 * ff_pad])
        gate, up = sums[:, 0:ff_pad], sums[:, ff_pad:]
        hidden = (gate / (1.0 + jnp.exp(-gate)) * up).astype(BF)
        part[:, 0:d_half] = dot_t(hidden, w[0, :, 2 * ff_pad :])
        part[:, d_half:] = dot_t(hidden, w[1, :, 2 * ff_pad :])

        @pl.when(i == 0)
        def _():
            own[...] = part[own_rows:, :]
            far_sum = part[0:own_rows, :].astype(BF)
            for way in range(2):
                sbuf[way, 0] = far_sum
                rs_copy(way, 0, False).start()

        @pl.when(i == 1)
        def _():
            for way in range(2):
                rs_copy(way, 0, False).wait_recv()

        @pl.when(i > 1)
        def _():
            for way in range(2):
                rs_copy(way, i - 1, True).wait_recv()

        @pl.when(i > 0)
        def _():
            for way in range(2):
                sbuf[way, i] = (rbuf[way, i - 1].astype(F32) + part[way * own_rows : (way + 1) * own_rows, :]).astype(BF)
                rs_copy(way, i, True).start()

        return unused

    lax.fori_loop(0, half_z, ring_step, 0)
    for way in range(2):
        rs_copy(way, half_z - 1, True).wait_recv()
    total = own[...] + rbuf[0, half_z - 1].astype(F32) + rbuf[1, half_z - 1].astype(F32)
    out_ref[...] = (stream[...] + swap_halves(total, False)).astype(out_ref.dtype)

    e_copy.wait_send()

    def g_sent(to, unused):
        g_copy(to).wait_send()
        return unused

    lax.fori_loop(z + 1, n_z, g_sent, 0)
    for m in range(3):

        def st_sent(j, unused, m=m):
            s, to = st_place(j)

            @pl.when(to != z)
            def _():
                st_copy(m, j, s, to).wait_send()

            return unused

        lax.fori_loop(0, tiles, st_sent, 0)
    for k in range(1, n_x):
        m_copy(k).wait_send()
    for way in range(2):
        for k in range(1, half_z + 1):
            ag_copy(way, k).wait_send()
        for i in range(half_z):
            rs_copy(way, i, i > 0).wait_send()
    for m in range(3):
        for r in range(4):
            s, valid = role(r)

            @pl.when(valid)
            def _(m=m, r=r, s=s):
                p_copy(m, r, s).wait_send()
                if r == 0:
                    xf_copy(m, 0, s).wait_send()
                    xf_copy(m, 1, s).wait_send()
                if r == 1:
                    xh_copy(m, 0, s).wait_send()
                if r == 3:
                    xh_copy(m, 1, s).wait_send()


def per_device(
    ssm_input, residual_in, log_step, decay_real, freq, in_real, in_imag, out_real, out_imag, skip,
    w_glu, b_glu, w_branch, norm_gain, w_gate, w_up, w_down,
):
    tok, width = ssm_input.shape
    groups, n_p = decay_real.shape
    group_size = in_real.shape[2]
    n_z, n_c, n_x = lax.axis_size("sp_0"), lax.axis_size("sp_1"), lax.axis_size("tp")
    d = residual_in.shape[1]
    wide = w_glu.shape[0]
    tiles = w_gate.shape[1] // LANES
    quads = n_z // n_x
    slots = -(-tiles // quads)
    assert n_c == 2 and n_x == 4 and slots < n_x and n_z % n_x == 0
    assert tok == SPAN * ROWS8 and 2 * n_p == LANES and w_gate.shape[1] % LANES == 0
    own_rows = tok // n_x
    n_state = groups * n_p
    half_z = n_z // 2
    vmem = pl.BlockSpec(memory_space=pltpu.VMEM)
    hbm = pl.BlockSpec(memory_space=pl.ANY)
    dma = pltpu.SemaphoreType.DMA
    return pl.pallas_call(
        functools.partial(kernel, (n_z, n_x, tiles, slots)),
        out_shape=jax.ShapeDtypeStruct((own_rows, d), BF),
        in_specs=[vmem] * 11 + [hbm] * 6,
        out_specs=vmem,
        scratch_shapes=[
            pltpu.VMEM((wide, wide), BF),
            pltpu.VMEM((wide, d), BF),
            pltpu.VMEM((own_rows, d), BF),
            pltpu.VMEM((2, d // 2, 3 * slots * LANES), BF),
            pltpu.VMEM((width, 2 * n_state), BF),
            pltpu.VMEM((width, 2 * n_state), BF),
            pltpu.VMEM((tok, 2 * n_state), F32),
            pltpu.VMEM((tok, 2 * n_state), BF),
            pltpu.VMEM((3, 2, n_state), F32),
            pltpu.VMEM((n_z, 2, n_state), F32),
            pltpu.VMEM((n_x, own_rows, width), BF),
            pltpu.VMEM((n_x, own_rows, width), BF),
            pltpu.VMEM((n_z, own_rows, d), BF),
            pltpu.VMEM((own_rows, d), F32),
            pltpu.VMEM((own_rows, d), F32),
            pltpu.VMEM((2 * own_rows, d), F32),
            pltpu.VMEM((2, half_z, own_rows, d), BF),
            pltpu.VMEM((2, half_z, own_rows, d), BF),
            dma((3,)), dma((3, tiles)), dma((3,)), dma((1,)), dma((1,)), dma((n_z,)), dma((n_z,)),
            dma((n_x,)), dma((n_x,)),
            dma((3, 2)), dma((3, 2)), dma((3, 2)), dma((3, 2)), dma((3, 4)), dma((3, 4)),
            dma((2, half_z)), dma((2, half_z)), dma((2, half_z)), dma((2, half_z)),
        ],
        compiler_params=pltpu.CompilerParams(collective_id=0, has_side_effects=True, vmem_limit_bytes=56 * 1024 * 1024),
        name="mixer_ffn",
    )(
        ssm_input,
        log_step.reshape(1, groups),
        decay_real,
        freq,
        in_real.transpose(0, 2, 1).reshape(groups * group_size, n_p),
        in_imag.transpose(0, 2, 1).reshape(groups * group_size, n_p),
        out_real.reshape(groups * group_size, n_p),
        out_imag.reshape(groups * group_size, n_p),
        skip.reshape(1, width),
        b_glu.reshape(1, wide),
        norm_gain.reshape(1, d),
        residual_in,
        w_glu,
        w_branch,
        w_gate,
        w_up,
        w_down.T,
    )


def solution(mesh):
    n_c = 2
    torus = Mesh(
        mesh.devices.reshape(mesh.shape["grp"], mesh.shape["sp"] // n_c, n_c, mesh.shape["tp"]),
        ("grp", "sp_0", "sp_1", "tp"),
    )
    in_specs = (
        P(GRP_SP, "tp"), P(GRP_SP, None), P("tp"), P("tp", None), P("tp", None),
        P("tp", None, None), P("tp", None, None), P("tp", None, None), P("tp", None, None), P("tp"),
        P(), P(), P(), P(), P(SP, "tp"), P(SP, "tp"), P("tp", SP),
    )
    return jax.shard_map(per_device, mesh=torus, in_specs=in_specs, out_specs=P(GRP_SP_TP, None), check_vma=False)
```

```python
import functools

import jax
import jax.numpy as jnp
from jax import lax
from jax.experimental import pallas as pl
from jax.experimental.pallas import tpu as pltpu
from jax.sharding import Mesh
from jax.sharding import PartitionSpec as P

SP = ("sp_0", "sp_1")
GRP_SP = ("grp", "sp_0", "sp_1")
GRP_SP_TP = ("grp", "sp_0", "sp_1", "tp")
EPS = 1e-06
LANES = 128
SPAN = 16
ROWS8 = 8
PARTS = 4
BF = jnp.bfloat16
F32 = jnp.float32
MESH = pl.DeviceIdType.MESH


def mod(a, n):
    return lax.rem(a + 8 * n, n)


def cmul(ar, ai, br, bi):
    return ar * br - ai * bi, ar * bi + ai * br


def dot(a, b):
    return jnp.dot(a, b, preferred_element_type=F32)


def dot_t(a, b):
    return lax.dot_general(a, b, (((1,), (1,)), ((), ())), preferred_element_type=F32)


def tile(v, k):
    return v[:, k * LANES : (k + 1) * LANES]


def swap_halves(v, forward):
    rows, width = v.shape
    half = width // LANES // 2
    low = lax.broadcasted_iota(jnp.int32, (rows, LANES), 1) < LANES // 2
    first, second = [], []
    for k in range(half):
        one, two = (tile(v, 2 * k), tile(v, 2 * k + 1)) if forward else (tile(v, k), tile(v, half + k))
        first.append(jnp.where(low, one, pltpu.roll(two, LANES // 2, 1)))
        second.append(jnp.where(low, pltpu.roll(one, LANES // 2, 1), two))
    if forward:
        return jnp.concatenate(first + second, axis=1)
    return jnp.concatenate([t for pair in zip(first, second) for t in pair], axis=1)


def kernel(
    dims,
    u_ref, ls_ref, dr_ref, fq_ref, inr_ref, ini_ref, our_ref, oui_ref, skip_ref, bglu_ref, gain_ref,
    resid_hbm, wglu_hbm, wbr_hbm, wg_hbm, wu_hbm, wd_hbm,
    out_ref,
    wglu, wbr, resid, packed, w, tab_b, tab_c, drive, states, est, gst, mo, mrecv, act, stream, own, part, sbuf, rbuf,
    cp_sem, st_sent, st_recv, e_send, e_recv, g_send, g_recv, m_send, m_recv,
    xf_send, xf_recv, xh_send, xh_recv, p_send, p_recv, ag_send, ag_recv, rs_send, rs_recv, pk_sem,
):
    n_z, n_x, tiles, slots = dims
    quads = n_z // n_x
    z, c, x = lax.axis_index("sp_0"), lax.axis_index("sp_1"), lax.axis_index("tp")
    zq = lax.div(z, n_x)
    right, left = {"sp_0": mod(z + 1, n_z)}, {"sp_0": mod(z - 1, n_z)}
    other = {"sp_1": 1 - c}
    tok, width = u_ref.shape
    groups, lanes_state = dr_ref.shape
    n_state = groups * lanes_state
    half_z = n_z // 2
    own_rows, d = stream.shape
    d_half = d // 2
    d_block = d_half // n_z
    ff_pad = slots * LANES

    barrier = pltpu.get_barrier_semaphore()

    def greet(k, unused):
        pl.semaphore_signal(barrier, inc=1, device_id={"sp_0": mod(z + k, n_z)}, device_id_type=MESH)
        return unused

    lax.fori_loop(1, n_z, greet, 0)
    for k in range(1, n_x):
        pl.semaphore_signal(barrier, inc=1, device_id={"tp": mod(x + k, n_x)}, device_id_type=MESH)
    pl.semaphore_signal(barrier, inc=1, device_id=other, device_id_type=MESH)

    local = [
        pltpu.make_async_copy(wglu_hbm, wglu, cp_sem.at[0]),
        pltpu.make_async_copy(wbr_hbm, wbr, cp_sem.at[1]),
        pltpu.make_async_copy(resid_hbm.at[pl.ds(pl.multiple_of(x * own_rows, own_rows), own_rows)], resid, cp_sem.at[2]),
    ]
    for copy in local:
        copy.start()
    packs = []
    for m, source in enumerate((wg_hbm, wu_hbm, wd_hbm)):
        for j in range(tiles):
            rows = pl.ds(m * d_block, d_block)
            packs.append(pltpu.make_async_copy(source.at[:, pl.ds(j * LANES, LANES)], packed.at[j, rows, :], pk_sem.at[m, j]))
    for copy in packs:
        copy.start()

    diag = lax.broadcasted_iota(jnp.int32, (groups, groups), 0) == lax.broadcasted_iota(jnp.int32, (groups, groups), 1)
    step = jnp.sum(jnp.where(diag, jnp.broadcast_to(jnp.exp(ls_ref[...]), (groups, groups)), 0.0), axis=1, keepdims=True)
    dr, fq = dr_ref[...], fq_ref[...]
    mag = jnp.exp(dr * step)
    abar_re, abar_im = mag * jnp.cos(fq * step), mag * jnp.sin(fq * step)
    denominator = dr * dr + fq * fq
    less_re = abar_re - 1.0
    hold_re = (less_re * dr + abar_im * fq) / denominator
    hold_im = (abar_im * dr - less_re * fq) / denominator

    def row_form(v):
        twice = jnp.concatenate([v, v], axis=1)
        row = lax.broadcasted_iota(jnp.int32, (groups, LANES), 0)
        lane = lax.broadcasted_iota(jnp.int32, (groups, LANES), 1)
        pieces = []
        for k in range(n_state // LANES):
            keep = row == 2 * k + lax.div(lane, lanes_state)
            pieces.append(jnp.sum(jnp.where(keep, twice, 0.0), axis=0, keepdims=True))
        return jnp.concatenate(pieces, axis=1)

    a_re, a_im = row_form(abar_re), row_form(abar_im)
    h_re, h_im = row_form(hold_re), row_form(hold_im)

    group_size = width // groups
    pair_rows = 2 * group_size
    row = lax.broadcasted_iota(jnp.int32, (pair_rows, LANES), 0)
    lane = lax.broadcasted_iota(jnp.int32, (pair_rows, LANES), 1)
    keep = lax.div(row, group_size) == lax.div(lane, lanes_state)

    tab_b[...] = jnp.zeros_like(tab_b)
    tab_c[...] = jnp.zeros_like(tab_c)

    def put(table, k, col, value):
        table[k * pair_rows : (k + 1) * pair_rows, col + k * LANES : col + (k + 1) * LANES] = jnp.where(keep, value, 0.0).astype(BF)

    def twice_of(ref, k):
        v = ref[k * pair_rows : (k + 1) * pair_rows, :]
        return jnp.concatenate([v, v], axis=1)

    for k in range(n_state // LANES):
        hr, hi = tile(h_re, k), tile(h_im, k)
        ir, ii = twice_of(inr_ref, k), twice_of(ini_ref, k)
        put(tab_b, k, 0, hr * ir - hi * ii)
        put(tab_b, k, n_state, hr * ii + hi * ir)
        put(tab_c, k, 0, twice_of(our_ref, k))
        put(tab_c, k, n_state, -twice_of(oui_ref, k))

    to_row = lax.broadcasted_iota(jnp.int32, (tok, tok), 0)
    to_col = lax.broadcasted_iota(jnp.int32, (tok, tok), 1)
    order = (to_col == lax.rem(to_row, ROWS8) * SPAN + lax.div(to_row, ROWS8)).astype(F32).astype(BF)
    back = (to_row == lax.rem(to_col, ROWS8) * SPAN + lax.div(to_col, ROWS8)).astype(F32).astype(BF)
    u_perm = dot(order, u_ref[...])
    drive[...] = dot(u_perm.astype(BF), tab_b[...])

    ar, ai = jnp.broadcast_to(a_re, (ROWS8, n_state)), jnp.broadcast_to(a_im, (ROWS8, n_state))
    s_re = drive[0:ROWS8, 0:n_state]
    s_im = drive[0:ROWS8, n_state:]
    for j in range(1, SPAN):
        at = slice(j * ROWS8, (j + 1) * ROWS8)
        p_re, p_im = cmul(ar, ai, s_re, s_im)
        s_re = p_re + drive[at, 0:n_state]
        s_im = p_im + drive[at, n_state:]
        drive[at, 0:n_state] = s_re
        drive[at, n_state:] = s_im

    pw = [(ar, ai)]
    for _ in range(8):
        pw.append(cmul(*pw[-1], *pw[-1]))
    chunk = lax.broadcasted_iota(jnp.int32, (ROWS8, n_state), 0)

    def shifted(v, by):
        return jnp.where(chunk >= by, pltpu.roll(v, by, 0), 0.0)

    i_re, i_im = s_re, s_im
    for level, by in ((4, 1), (5, 2), (6, 4)):
        q_re, q_im = cmul(*pw[level], shifted(i_re, by), shifted(i_im, by))
        i_re, i_im = i_re + q_re, i_im + q_im
    before_re, before_im = shifted(i_re, 1), shifted(i_im, 1)
    end_re, end_im = i_re[ROWS8 - 1 :, :], i_im[ROWS8 - 1 :, :]
    est[0, 0:1, :] = end_re
    est[0, 1:2, :] = end_im
    a128 = (pw[7][0][0:1], pw[7][1][0:1])
    a256 = (pw[8][0][0:1], pw[8][1][0:1])

    for s in range(slots):
        if s * quads + quads - 1 >= tiles:

            @pl.when(s * quads + zq >= tiles)
            def _():
                w[s] = jnp.zeros((2, n_z, 3 * d_block, LANES), BF)

    pl.semaphore_wait(barrier, n_z - 1 + n_x - 1 + 1)

    e_copy = pltpu.make_async_remote_copy(
        src_ref=est.at[0], dst_ref=est.at[1], send_sem=e_send.at[0], recv_sem=e_recv.at[0], device_id=other, device_id_type=MESH
    )
    e_copy.start()
    e_copy.wait_recv()
    oth_re, oth_im = est[1, 0:1, :], est[1, 1:2, :]
    first = c == 0
    e0_re, e0_im = jnp.where(first, end_re, oth_re), jnp.where(first, end_im, oth_im)
    e1_re, e1_im = jnp.where(first, oth_re, end_re), jnp.where(first, oth_im, end_im)
    g_re, g_im = cmul(*a128, e0_re, e0_im)
    est[2, 0:1, :] = g_re + e1_re
    est[2, 1:2, :] = g_im + e1_im

    def g_copy(to):
        return pltpu.make_async_remote_copy(
            src_ref=est.at[2], dst_ref=gst.at[z], send_sem=g_send.at[to], recv_sem=g_recv.at[z],
            device_id={"sp_0": to}, device_id_type=MESH,
        )

    def g_start(to, unused):
        g_copy(to).start()
        return unused

    lax.fori_loop(z + 1, n_z, g_start, 0)

    def tile_of(chip):
        s = mod(x - chip, n_x)
        return s, s * quads + lax.div(chip, n_x)

    def st_copy(chip, s, j):
        return pltpu.make_async_remote_copy(
            src_ref=packed.at[j], dst_ref=w.at[s, c, z], send_sem=st_sent.at[chip], recv_sem=st_recv.at[z],
            device_id={"sp_0": chip}, device_id_type=MESH,
        )

    def st_chip(k):
        up = half_z - lax.div(k, 2)
        return mod(jnp.where(lax.rem(k, 2) == 0, z + up, z - up + 1), n_z)

    def st_start(k, unused):
        chip = st_chip(k)
        s, j = tile_of(chip)

        @pl.when(j < tiles)
        def _():
            st_copy(chip, s, j).start()

        return unused

    for copy in packs:
        copy.wait()
    lax.fori_loop(0, n_z - 1, st_start, 0)
    s_mine, j_mine = tile_of(z)

    @pl.when(j_mine < tiles)
    def _():
        w[s_mine, c, z] = packed[j_mine]

    def add_state(frm, carry):
        g_got = pltpu.make_async_remote_copy(
            src_ref=est.at[2], dst_ref=gst.at[frm], send_sem=g_send.at[frm], recv_sem=g_recv.at[frm],
            device_id={"sp_0": frm}, device_id_type=MESH,
        )
        g_got.wait_recv()
        n_re, n_im = cmul(*a256, *carry)
        return n_re + gst[frm, 0:1, :], n_im + gst[frm, 1:2, :]

    zero_row = jnp.zeros((1, n_state), F32)
    in_re, in_im = lax.fori_loop(0, z, add_state, (zero_row, zero_row))
    t_re, t_im = cmul(*a128, in_re, in_im)
    in_re, in_im = jnp.where(first, in_re, t_re + oth_re), jnp.where(first, in_im, t_im + oth_im)

    one, nil = jnp.ones((ROWS8, n_state), F32), jnp.zeros((ROWS8, n_state), F32)
    r_re, r_im = one, nil
    for level, bit in ((4, 1), (5, 2), (6, 4)):
        has = lax.rem(lax.div(chunk, bit), 2) == 1
        r_re, r_im = cmul(r_re, r_im, jnp.where(has, pw[level][0], one), jnp.where(has, pw[level][1], nil))
    c_re, c_im = cmul(r_re, r_im, jnp.broadcast_to(in_re, (ROWS8, n_state)), jnp.broadcast_to(in_im, (ROWS8, n_state)))
    c_re, c_im = c_re + before_re, c_im + before_im
    for jj in range(SPAN // 2):
        out_re, out_im = [], []
        for j in (2 * jj, 2 * jj + 1):
            at = slice(j * ROWS8, (j + 1) * ROWS8)
            c_re, c_im = cmul(ar, ai, c_re, c_im)
            out_re.append(drive[at, 0:n_state] + c_re)
            out_im.append(drive[at, n_state:] + c_im)
        at = slice(2 * jj * ROWS8, 2 * (jj + 1) * ROWS8)
        states[at, 0:n_state] = jnp.concatenate(out_re, axis=0).astype(BF)
        states[at, n_state:] = jnp.concatenate(out_im, axis=0).astype(BF)
    values = dot_t(states[...], tab_c[...]) + skip_ref[...] * u_perm
    cubic = 0.7978845608028654 * (values + 0.044715 * (values * values * values))
    values = values * (0.5 * (1.0 + jnp.tanh(cubic)))
    mixed = dot(back, values.astype(BF)).astype(BF)
    for k in range(n_x):
        mo[k] = mixed[k * own_rows : (k + 1) * own_rows, :]

    def m_copy(k):
        to = mod(x + k, n_x)
        return pltpu.make_async_remote_copy(
            src_ref=mo.at[to], dst_ref=mrecv.at[x], send_sem=m_send.at[k], recv_sem=m_recv.at[k],
            device_id={"tp": to}, device_id_type=MESH,
        )

    for k in range(1, n_x):
        m_copy(k).start()
    mrecv[x] = mo[x]
    for copy in local:
        copy.wait()
    for k in range(1, n_x):
        m_copy(k).wait_recv()
    rows_in = jnp.concatenate([mrecv[k] for k in range(n_x)], axis=1)
    glu = dot(rows_in, wglu[...]) + bglu_ref[...]
    gated = (rows_in.astype(F32) / (1.0 + jnp.exp(-glu))).astype(BF)
    st = resid[...].astype(F32) + dot(gated, wbr[...])
    stream[...] = st
    scale = lax.rsqrt(jnp.mean(st * st, axis=-1, keepdims=True) + EPS)
    act[z] = swap_halves(st * scale * gain_ref[...], True).astype(BF)

    half_rows = own_rows // 2

    wide_part = d // PARTS

    def remote(ref, send, recv, to):
        return pltpu.make_async_remote_copy(
            src_ref=ref, dst_ref=ref, send_sem=send, recv_sem=recv, device_id=to, device_id_type=MESH
        )

    def ag_ref(way, k, q, block):
        rows = pl.ds(0, own_rows) if k < half_z else pl.ds(way * half_rows, half_rows)
        return act.at[block, rows, pl.ds(q * wide_part, wide_part)]

    def ag_copy(way, k, q):
        to, block = (right, mod(z - k + 1, n_z)) if way == 0 else (left, mod(z + k - 1, n_z))
        return remote(ag_ref(way, k, q, block), ag_send.at[way, k - 1, q], ag_recv.at[way, k - 1, q], to)

    def ag_got(way, k, q):
        block = mod(z - k, n_z) if way == 0 else mod(z + k, n_z)
        return remote(ag_ref(way, k, q, block), ag_send.at[way, k - 1, q], ag_recv.at[way, k - 1, q], right)

    def ag_start(k):
        for q in range(PARTS):
            for way in range(2):
                ag_copy(way, k, q).start()

    def ag_next(k):
        for q in range(PARTS):
            for way in range(2):
                ag_got(way, k, q).wait_recv()
                if k < half_z:
                    ag_copy(way, k + 1, q).start()

    def role(r):
        s = mod(x - z - r, n_x)
        return s, s * quads + zq < tiles

    x_to = {0: {"tp": mod(x + 1, n_x)}, 1: {"tp": mod(x - 1, n_x)}}
    fours = n_z // 4

    def group(core, s, g):
        return w.at[s, core, pl.ds(g * fours, fours)]

    def xf_copy(g, way, s):
        return remote(group(c, s, g), xf_send.at[g, way], xf_recv.at[g, way], x_to[way])

    def xh_copy(g, s):
        return remote(group(c, s, g), xh_send.at[g], xh_recv.at[g], x_to[g // 2])

    def p_copy(g, r, s):
        return remote(group(c, s, g), p_send.at[g, r], p_recv.at[g, r], other)

    def x_owner(g):
        s, valid = role(0)

        @pl.when(valid)
        def _():
            for chip in range(g * fours, (g + 1) * fours):

                @pl.when(z != chip)
                def _(chip=chip):
                    remote(w.at[s, c, chip], st_sent.at[chip], st_recv.at[chip], right).wait_recv()

            for way in range(2):
                xf_copy(g, way, s).start()
            p_copy(g, 0, s).start()

    def x_relay(g):
        for way, r in ((0, 1), (1, 3)):
            s, valid = role(r)

            @pl.when(valid)
            def _(way=way, r=r, s=s):
                xf_copy(g, way, s).wait_recv()
                if g // 2 == way:
                    xh_copy(g, s).start()
                p_copy(g, r, s).start()

    def x_last(g):
        s, valid = role(2)

        @pl.when(valid)
        def _():
            xh_copy(g, s).wait_recv()
            p_copy(g, 2, s).start()

    def x_partner(g):
        for r in range(4):
            s, valid = role(r)

            @pl.when(valid)
            def _(r=r, s=s):
                remote(group(1 - c, s, g), p_send.at[g, r], p_recv.at[g, r], other).wait_recv()

    ag_start(1)
    after = {
        0: [(x_owner, 0), (x_owner, 1)],
        1: [(x_owner, 2)],
        2: [(x_owner, 3)],
        3: [(x_relay, 0)],
        4: [(x_relay, 1)],
        5: [(x_relay, 2), (x_last, 0)],
        6: [(x_relay, 3), (x_last, 1)],
        7: [(x_last, 2)],
        8: [(x_last, 3)] + [(x_partner, g) for g in range(4)],
    }
    for k in range(half_z + 1):
        if k:
            ag_next(k)
        for what, g in after.get(k, ()):
            what(g)

    rbuf[0, 0, half_rows:, :] = jnp.zeros((own_rows - half_rows, d), BF)
    rbuf[1, 0, 0:half_rows, :] = jnp.zeros((half_rows, d), BF)

    def rs_copy(way, i, q, whole):
        rows = pl.ds(0, own_rows) if whole else pl.ds(way * half_rows, half_rows)
        lanes = pl.ds(q * wide_part, wide_part)
        return pltpu.make_async_remote_copy(
            src_ref=sbuf.at[way, i, rows, lanes], dst_ref=rbuf.at[way, i, rows, lanes],
            send_sem=rs_send.at[way, i, q], recv_sem=rs_recv.at[way, i, q],
            device_id=right if way == 0 else left, device_id_type=MESH,
        )

    def matrix(core, kinds):
        at = [(m * d_block, s) for m in kinds for s in range(slots)]
        return jnp.concatenate([w[s, core, :, r : r + d_block, :].reshape(d_half, LANES) for r, s in at], axis=1)

    def ring_step(i, unused):
        far = half_z - i
        one_at = mod(z + far, n_z)
        two_at = jnp.where(i == 0, z, mod(z - far, n_z))
        rows2 = jnp.concatenate([act[one_at], act[two_at]], axis=0)
        sums = dot(rows2[:, 0:d_half], matrix(0, (0, 1))) + dot(rows2[:, d_half:], matrix(1, (0, 1)))
        gate, up = sums[:, 0:ff_pad], sums[:, ff_pad:]
        hidden = (gate / (1.0 + jnp.exp(-gate)) * up).astype(BF)
        part[:, 0:d_half] = dot_t(hidden, matrix(0, (2,)))
        part[:, d_half:] = dot_t(hidden, matrix(1, (2,)))

        @pl.when(i == 0)
        def _():
            own[...] = part[own_rows:, :]
            far_sum = part[0:own_rows, :].astype(BF)
            for way in range(2):
                sbuf[way, 0] = far_sum
            for q in range(PARTS):
                for way in range(2):
                    rs_copy(way, 0, q, False).start()

        def pass_on(i, whole):
            for q in range(PARTS):
                lanes = slice(q * wide_part, (q + 1) * wide_part)
                for way in range(2):
                    rs_copy(way, i - 1, q, whole).wait_recv()
                    mine = part[way * own_rows : (way + 1) * own_rows, lanes]
                    sbuf[way, i, :, lanes] = (rbuf[way, i - 1, :, lanes].astype(F32) + mine).astype(BF)
                    rs_copy(way, i, q, True).start()

        @pl.when(i == 1)
        def _():
            pass_on(1, False)

        @pl.when(i > 1)
        def _():
            pass_on(i, True)

        return unused

    lax.fori_loop(0, half_z, ring_step, 0)
    for way in range(2):
        for q in range(PARTS):
            rs_copy(way, half_z - 1, q, True).wait_recv()
    total = own[...] + rbuf[0, half_z - 1].astype(F32) + rbuf[1, half_z - 1].astype(F32)
    out_ref[...] = (stream[...] + swap_halves(total, False)).astype(out_ref.dtype)

    e_copy.wait_send()

    def g_sent(to, unused):
        g_copy(to).wait_send()
        return unused

    lax.fori_loop(z + 1, n_z, g_sent, 0)

    def st_left(k, unused):
        chip = st_chip(k)
        s, j = tile_of(chip)

        @pl.when(j < tiles)
        def _():
            st_copy(chip, s, j).wait_send()

        return unused

    lax.fori_loop(0, n_z - 1, st_left, 0)
    for k in range(1, n_x):
        m_copy(k).wait_send()
    for way in range(2):
        for k in range(1, half_z + 1):
            for q in range(PARTS):
                ag_copy(way, k, q).wait_send()
        for i in range(half_z):
            for q in range(PARTS):
                rs_copy(way, i, q, i > 0).wait_send()
    for g in range(4):
        for r in range(4):
            s, valid = role(r)

            @pl.when(valid)
            def _(g=g, r=r, s=s):
                p_copy(g, r, s).wait_send()
                if r == 0:
                    xf_copy(g, 0, s).wait_send()
                    xf_copy(g, 1, s).wait_send()
                if (r, g // 2) in ((1, 0), (3, 1)):
                    xh_copy(g, s).wait_send()


def per_device(
    ssm_input, residual_in, log_step, decay_real, freq, in_real, in_imag, out_real, out_imag, skip,
    w_glu, b_glu, w_branch, norm_gain, w_gate, w_up, w_down,
):
    tok, width = ssm_input.shape
    groups, n_p = decay_real.shape
    group_size = in_real.shape[2]
    n_z, n_c, n_x = lax.axis_size("sp_0"), lax.axis_size("sp_1"), lax.axis_size("tp")
    d = residual_in.shape[1]
    wide = w_glu.shape[0]
    tiles = w_gate.shape[1] // LANES
    quads = n_z // n_x
    slots = -(-tiles // quads)
    assert n_c == 2 and n_x == 4 and slots < n_x and n_z % n_x == 0
    assert tok == SPAN * ROWS8 and 2 * n_p == LANES and w_gate.shape[1] % LANES == 0
    own_rows = tok // n_x
    n_state = groups * n_p
    half_z = n_z // 2
    vmem = pl.BlockSpec(memory_space=pltpu.VMEM)
    hbm = pl.BlockSpec(memory_space=pl.ANY)
    dma = pltpu.SemaphoreType.DMA
    return pl.pallas_call(
        functools.partial(kernel, (n_z, n_x, tiles, slots)),
        out_shape=jax.ShapeDtypeStruct((own_rows, d), BF),
        in_specs=[vmem] * 11 + [hbm] * 6,
        out_specs=vmem,
        scratch_shapes=[
            pltpu.VMEM((wide, wide), BF),
            pltpu.VMEM((wide, d), BF),
            pltpu.VMEM((own_rows, d), BF),
            pltpu.VMEM((tiles, 3 * w_gate.shape[0], LANES), BF),
            pltpu.VMEM((slots, 2, n_z, 3 * w_gate.shape[0], LANES), BF),
            pltpu.VMEM((width, 2 * n_state), BF),
            pltpu.VMEM((width, 2 * n_state), BF),
            pltpu.VMEM((tok, 2 * n_state), F32),
            pltpu.VMEM((tok, 2 * n_state), BF),
            pltpu.VMEM((3, 2, n_state), F32),
            pltpu.VMEM((n_z, 2, n_state), F32),
            pltpu.VMEM((n_x, own_rows, width), BF),
            pltpu.VMEM((n_x, own_rows, width), BF),
            pltpu.VMEM((n_z, own_rows, d), BF),
            pltpu.VMEM((own_rows, d), F32),
            pltpu.VMEM((own_rows, d), F32),
            pltpu.VMEM((2 * own_rows, d), F32),
            pltpu.VMEM((2, half_z, own_rows, d), BF),
            pltpu.VMEM((2, half_z, own_rows, d), BF),
            dma((3,)), dma((n_z,)), dma((n_z,)), dma((1,)), dma((1,)), dma((n_z,)), dma((n_z,)),
            dma((n_x,)), dma((n_x,)),
            dma((4, 2)), dma((4, 2)), dma((4,)), dma((4,)), dma((4, 4)), dma((4, 4)),
            dma((2, half_z, PARTS)), dma((2, half_z, PARTS)), dma((2, half_z, PARTS)), dma((2, half_z, PARTS)),
            dma((3, tiles)),
        ],
        compiler_params=pltpu.CompilerParams(collective_id=0, has_side_effects=True, vmem_limit_bytes=56 * 1024 * 1024),
        name="mixer_ffn",
    )(
        ssm_input,
        log_step.reshape(1, groups),
        decay_real,
        freq,
        in_real.transpose(0, 2, 1).reshape(groups * group_size, n_p),
        in_imag.transpose(0, 2, 1).reshape(groups * group_size, n_p),
        out_real.reshape(groups * group_size, n_p),
        out_imag.reshape(groups * group_size, n_p),
        skip.reshape(1, width),
        b_glu.reshape(1, wide),
        norm_gain.reshape(1, d),
        residual_in,
        w_glu,
        w_branch,
        w_gate,
        w_up,
        w_down.T,
    )


def solution(mesh):
    n_c = 2
    torus = Mesh(
        mesh.devices.reshape(mesh.shape["grp"], mesh.shape["sp"] // n_c, n_c, mesh.shape["tp"]),
        ("grp", "sp_0", "sp_1", "tp"),
    )
    in_specs = (
        P(GRP_SP, "tp"), P(GRP_SP, None), P("tp"), P("tp", None), P("tp", None),
        P("tp", None, None), P("tp", None, None), P("tp", None, None), P("tp", None, None), P("tp"),
        P(), P(), P(), P(), P(SP, "tp"), P(SP, "tp"), P("tp", SP),
    )
    return jax.shard_map(per_device, mesh=torus, in_specs=in_specs, out_specs=P(GRP_SP_TP, None), check_vma=False)
```

```python
import functools

import jax
import jax.numpy as jnp
from jax import lax
from jax.experimental import pallas as pl
from jax.experimental.pallas import tpu as pltpu
from jax.sharding import Mesh
from jax.sharding import PartitionSpec as P

SP = ("sp_0", "sp_1")
GRP_SP = ("grp", "sp_0", "sp_1")
GRP_SP_TP = ("grp", "sp_0", "sp_1", "tp")
EPS = 1e-06
LANES = 128
SPAN = 16
ROWS8 = 8
PARTS = 4
BF = jnp.bfloat16
F32 = jnp.float32
MESH = pl.DeviceIdType.MESH


def mod(a, n):
    return lax.rem(a + 8 * n, n)


def cmul(ar, ai, br, bi):
    return ar * br - ai * bi, ar * bi + ai * br


def dot(a, b):
    return jnp.dot(a, b, preferred_element_type=F32)


def dot_t(a, b):
    return lax.dot_general(a, b, (((1,), (1,)), ((), ())), preferred_element_type=F32)


def tile(v, k):
    return v[:, k * LANES : (k + 1) * LANES]


def swap_halves(v, forward):
    rows, width = v.shape
    half = width // LANES // 2
    low = lax.broadcasted_iota(jnp.int32, (rows, LANES), 1) < LANES // 2
    first, second = [], []
    for k in range(half):
        one, two = (tile(v, 2 * k), tile(v, 2 * k + 1)) if forward else (tile(v, k), tile(v, half + k))
        first.append(jnp.where(low, one, pltpu.roll(two, LANES // 2, 1)))
        second.append(jnp.where(low, pltpu.roll(one, LANES // 2, 1), two))
    if forward:
        return jnp.concatenate(first + second, axis=1)
    return jnp.concatenate([t for pair in zip(first, second) for t in pair], axis=1)


def kernel(
    dims,
    u_ref, ls_ref, dr_ref, fq_ref, inr_ref, ini_ref, our_ref, oui_ref, skip_ref, bglu_ref, gain_ref,
    resid_hbm, wglu_hbm, wbr_hbm, wg_hbm, wu_hbm, wd_hbm,
    out_ref,
    wglu, wbr, resid, packed, w, tab_b, tab_c, drive, states, est, gst, mo, mrecv, act, stream, own, part, sbuf, rbuf,
    cp_sem, st_sent, st_recv, e_send, e_recv, g_send, g_recv, m_send, m_recv,
    xf_send, xf_recv, xh_send, xh_recv, p_send, p_recv, ag_send, ag_recv, rs_send, rs_recv, pk_sem,
):
    n_z, n_x, tiles, slots = dims
    quads = n_z // n_x
    z, c, x = lax.axis_index("sp_0"), lax.axis_index("sp_1"), lax.axis_index("tp")
    zq = lax.div(z, n_x)
    right, left = {"sp_0": mod(z + 1, n_z)}, {"sp_0": mod(z - 1, n_z)}
    other = {"sp_1": 1 - c}
    tok, width = u_ref.shape
    groups, lanes_state = dr_ref.shape
    n_state = groups * lanes_state
    half_z = n_z // 2
    own_rows, d = stream.shape
    d_half = d // 2
    d_block = d_half // n_z
    ff_pad = slots * LANES

    barrier = pltpu.get_barrier_semaphore()

    def greet(k, unused):
        pl.semaphore_signal(barrier, inc=1, device_id={"sp_0": mod(z + k, n_z)}, device_id_type=MESH)
        return unused

    lax.fori_loop(1, n_z, greet, 0)
    for k in range(1, n_x):
        pl.semaphore_signal(barrier, inc=1, device_id={"tp": mod(x + k, n_x)}, device_id_type=MESH)
    pl.semaphore_signal(barrier, inc=1, device_id=other, device_id_type=MESH)

    local = [
        pltpu.make_async_copy(wglu_hbm, wglu, cp_sem.at[0]),
        pltpu.make_async_copy(wbr_hbm, wbr, cp_sem.at[1]),
        pltpu.make_async_copy(resid_hbm.at[pl.ds(pl.multiple_of(x * own_rows, own_rows), own_rows)], resid, cp_sem.at[2]),
    ]
    for copy in local:
        copy.start()
    packs = []
    for m, source in enumerate((wg_hbm, wu_hbm, wd_hbm)):
        for j in range(tiles):
            rows = pl.ds(m * d_block, d_block)
            packs.append(pltpu.make_async_copy(source.at[:, pl.ds(j * LANES, LANES)], packed.at[j, rows, :], pk_sem.at[m, j]))
    for copy in packs:
        copy.start()

    diag = lax.broadcasted_iota(jnp.int32, (groups, groups), 0) == lax.broadcasted_iota(jnp.int32, (groups, groups), 1)
    step = jnp.sum(jnp.where(diag, jnp.broadcast_to(jnp.exp(ls_ref[...]), (groups, groups)), 0.0), axis=1, keepdims=True)
    dr, fq = dr_ref[...], fq_ref[...]
    mag = jnp.exp(dr * step)
    abar_re, abar_im = mag * jnp.cos(fq * step), mag * jnp.sin(fq * step)
    denominator = dr * dr + fq * fq
    less_re = abar_re - 1.0
    hold_re = (less_re * dr + abar_im * fq) / denominator
    hold_im = (abar_im * dr - less_re * fq) / denominator

    def row_form(v):
        twice = jnp.concatenate([v, v], axis=1)
        row = lax.broadcasted_iota(jnp.int32, (groups, LANES), 0)
        lane = lax.broadcasted_iota(jnp.int32, (groups, LANES), 1)
        pieces = []
        for k in range(n_state // LANES):
            keep = row == 2 * k + lax.div(lane, lanes_state)
            pieces.append(jnp.sum(jnp.where(keep, twice, 0.0), axis=0, keepdims=True))
        return jnp.concatenate(pieces, axis=1)

    a_re, a_im = row_form(abar_re), row_form(abar_im)
    h_re, h_im = row_form(hold_re), row_form(hold_im)

    group_size = width // groups
    pair_rows = 2 * group_size
    row = lax.broadcasted_iota(jnp.int32, (pair_rows, LANES), 0)
    lane = lax.broadcasted_iota(jnp.int32, (pair_rows, LANES), 1)
    keep = lax.div(row, group_size) == lax.div(lane, lanes_state)

    tab_b[...] = jnp.zeros_like(tab_b)

    def put(table, k, col, value):
        table[k * pair_rows : (k + 1) * pair_rows, col + k * LANES : col + (k + 1) * LANES] = jnp.where(keep, value, 0.0).astype(BF)

    def twice_of(ref, k):
        v = ref[k * pair_rows : (k + 1) * pair_rows, :]
        return jnp.concatenate([v, v], axis=1)

    for k in range(n_state // LANES):
        hr, hi = tile(h_re, k), tile(h_im, k)
        ir, ii = twice_of(inr_ref, k), twice_of(ini_ref, k)
        put(tab_b, k, 0, hr * ir - hi * ii)
        put(tab_b, k, n_state, hr * ii + hi * ir)

    to_row = lax.broadcasted_iota(jnp.int32, (tok, tok), 0)
    to_col = lax.broadcasted_iota(jnp.int32, (tok, tok), 1)
    order = (to_col == lax.rem(to_row, ROWS8) * SPAN + lax.div(to_row, ROWS8)).astype(F32).astype(BF)
    back = (to_row == lax.rem(to_col, ROWS8) * SPAN + lax.div(to_col, ROWS8)).astype(F32).astype(BF)
    u_perm = dot(order, u_ref[...])
    drive[...] = dot(u_perm.astype(BF), tab_b[...])

    ar, ai = jnp.broadcast_to(a_re, (ROWS8, n_state)), jnp.broadcast_to(a_im, (ROWS8, n_state))
    s_re = drive[0:ROWS8, 0:n_state]
    s_im = drive[0:ROWS8, n_state:]
    for j in range(1, SPAN):
        at = slice(j * ROWS8, (j + 1) * ROWS8)
        p_re, p_im = cmul(ar, ai, s_re, s_im)
        s_re = p_re + drive[at, 0:n_state]
        s_im = p_im + drive[at, n_state:]
        drive[at, 0:n_state] = s_re
        drive[at, n_state:] = s_im

    pw = [(ar, ai)]
    for _ in range(8):
        pw.append(cmul(*pw[-1], *pw[-1]))
    chunk = lax.broadcasted_iota(jnp.int32, (ROWS8, n_state), 0)

    def shifted(v, by):
        return jnp.where(chunk >= by, pltpu.roll(v, by, 0), 0.0)

    i_re, i_im = s_re, s_im
    for level, by in ((4, 1), (5, 2), (6, 4)):
        q_re, q_im = cmul(*pw[level], shifted(i_re, by), shifted(i_im, by))
        i_re, i_im = i_re + q_re, i_im + q_im
    before_re, before_im = shifted(i_re, 1), shifted(i_im, 1)
    end_re, end_im = i_re[ROWS8 - 1 :, :], i_im[ROWS8 - 1 :, :]
    est[0, 0:1, :] = end_re
    est[0, 1:2, :] = end_im
    a128 = (pw[7][0][0:1], pw[7][1][0:1])
    a256 = (pw[8][0][0:1], pw[8][1][0:1])

    for s in range(slots):
        if s * quads + quads - 1 >= tiles:

            @pl.when(s * quads + zq >= tiles)
            def _():
                w[s] = jnp.zeros((2, n_z, 3 * d_block, LANES), BF)

    pl.semaphore_wait(barrier, n_z - 1 + n_x - 1 + 1)

    e_copy = pltpu.make_async_remote_copy(
        src_ref=est.at[0], dst_ref=est.at[1], send_sem=e_send.at[0], recv_sem=e_recv.at[0], device_id=other, device_id_type=MESH
    )
    e_copy.start()
    e_copy.wait_recv()
    oth_re, oth_im = est[1, 0:1, :], est[1, 1:2, :]
    first = c == 0
    e0_re, e0_im = jnp.where(first, end_re, oth_re), jnp.where(first, end_im, oth_im)
    e1_re, e1_im = jnp.where(first, oth_re, end_re), jnp.where(first, oth_im, end_im)
    g_re, g_im = cmul(*a128, e0_re, e0_im)
    est[2, 0:1, :] = g_re + e1_re
    est[2, 1:2, :] = g_im + e1_im

    def g_copy(to):
        return pltpu.make_async_remote_copy(
            src_ref=est.at[2], dst_ref=gst.at[z], send_sem=g_send.at[to], recv_sem=g_recv.at[z],
            device_id={"sp_0": to}, device_id_type=MESH,
        )

    def g_start(to, unused):
        g_copy(to).start()
        return unused

    lax.fori_loop(z + 1, n_z, g_start, 0)

    def tile_of(chip):
        s = mod(x - chip, n_x)
        return s, s * quads + lax.div(chip, n_x)

    def st_copy(chip, s, j):
        return pltpu.make_async_remote_copy(
            src_ref=packed.at[j], dst_ref=w.at[s, c, z], send_sem=st_sent.at[chip], recv_sem=st_recv.at[z],
            device_id={"sp_0": chip}, device_id_type=MESH,
        )

    def st_chip(k):
        up = lax.div(k, 2) + 1
        return mod(jnp.where(lax.rem(k, 2) == 0, z + up, z - up), n_z)

    def st_start(k, unused):
        chip = st_chip(k)
        s, j = tile_of(chip)

        @pl.when(j < tiles)
        def _():
            st_copy(chip, s, j).start()

        return unused

    for copy in packs:
        copy.wait()
    lax.fori_loop(0, n_z - 1, st_start, 0)
    s_mine, j_mine = tile_of(z)

    @pl.when(j_mine < tiles)
    def _():
        w[s_mine, c, z] = packed[j_mine]

    tab_c[...] = jnp.zeros_like(tab_c)
    for k in range(n_state // LANES):
        put(tab_c, k, 0, twice_of(our_ref, k))
        put(tab_c, k, n_state, -twice_of(oui_ref, k))

    def add_state(frm, carry):
        g_got = pltpu.make_async_remote_copy(
            src_ref=est.at[2], dst_ref=gst.at[frm], send_sem=g_send.at[frm], recv_sem=g_recv.at[frm],
            device_id={"sp_0": frm}, device_id_type=MESH,
        )
        g_got.wait_recv()
        n_re, n_im = cmul(*a256, *carry)
        return n_re + gst[frm, 0:1, :], n_im + gst[frm, 1:2, :]

    zero_row = jnp.zeros((1, n_state), F32)
    in_re, in_im = lax.fori_loop(0, z, add_state, (zero_row, zero_row))
    t_re, t_im = cmul(*a128, in_re, in_im)
    in_re, in_im = jnp.where(first, in_re, t_re + oth_re), jnp.where(first, in_im, t_im + oth_im)

    one, nil = jnp.ones((ROWS8, n_state), F32), jnp.zeros((ROWS8, n_state), F32)
    r_re, r_im = one, nil
    for level, bit in ((4, 1), (5, 2), (6, 4)):
        has = lax.rem(lax.div(chunk, bit), 2) == 1
        r_re, r_im = cmul(r_re, r_im, jnp.where(has, pw[level][0], one), jnp.where(has, pw[level][1], nil))
    c_re, c_im = cmul(r_re, r_im, jnp.broadcast_to(in_re, (ROWS8, n_state)), jnp.broadcast_to(in_im, (ROWS8, n_state)))
    c_re, c_im = c_re + before_re, c_im + before_im
    for jj in range(SPAN // 2):
        out_re, out_im = [], []
        for j in (2 * jj, 2 * jj + 1):
            at = slice(j * ROWS8, (j + 1) * ROWS8)
            c_re, c_im = cmul(ar, ai, c_re, c_im)
            out_re.append(drive[at, 0:n_state] + c_re)
            out_im.append(drive[at, n_state:] + c_im)
        at = slice(2 * jj * ROWS8, 2 * (jj + 1) * ROWS8)
        states[at, 0:n_state] = jnp.concatenate(out_re, axis=0).astype(BF)
        states[at, n_state:] = jnp.concatenate(out_im, axis=0).astype(BF)
    values = dot_t(states[...], tab_c[...]) + skip_ref[...] * u_perm
    cubic = 0.7978845608028654 * (values + 0.044715 * (values * values * values))
    values = values * (0.5 * (1.0 + jnp.tanh(cubic)))
    mixed = dot(back, values.astype(BF)).astype(BF)
    for k in range(n_x):
        mo[k] = mixed[k * own_rows : (k + 1) * own_rows, :]

    def m_copy(k):
        to = mod(x + k, n_x)
        return pltpu.make_async_remote_copy(
            src_ref=mo.at[to], dst_ref=mrecv.at[x], send_sem=m_send.at[k], recv_sem=m_recv.at[k],
            device_id={"tp": to}, device_id_type=MESH,
        )

    for k in range(1, n_x):
        m_copy(k).start()
    mrecv[x] = mo[x]
    for copy in local:
        copy.wait()
    for k in range(1, n_x):
        m_copy(k).wait_recv()
    rows_in = jnp.concatenate([mrecv[k] for k in range(n_x)], axis=1)
    glu = dot(rows_in, wglu[...]) + bglu_ref[...]
    gated = (rows_in.astype(F32) / (1.0 + jnp.exp(-glu))).astype(BF)
    st = resid[...].astype(F32) + dot(gated, wbr[...])
    stream[...] = st
    scale = lax.rsqrt(jnp.mean(st * st, axis=-1, keepdims=True) + EPS)
    act[z] = swap_halves(st * scale * gain_ref[...], True).astype(BF)

    half_rows = own_rows // 2

    wide_part = d // PARTS

    def remote(ref, send, recv, to):
        return pltpu.make_async_remote_copy(
            src_ref=ref, dst_ref=ref, send_sem=send, recv_sem=recv, device_id=to, device_id_type=MESH
        )

    def ag_ref(way, k, q, block):
        rows = pl.ds(0, own_rows) if k < half_z else pl.ds(way * half_rows, half_rows)
        return act.at[block, rows, pl.ds(q * wide_part, wide_part)]

    def ag_copy(way, k, q):
        to, block = (right, mod(z - k + 1, n_z)) if way == 0 else (left, mod(z + k - 1, n_z))
        return remote(ag_ref(way, k, q, block), ag_send.at[way, k - 1, q], ag_recv.at[way, k - 1, q], to)

    def ag_got(way, k, q):
        block = mod(z - k, n_z) if way == 0 else mod(z + k, n_z)
        return remote(ag_ref(way, k, q, block), ag_send.at[way, k - 1, q], ag_recv.at[way, k - 1, q], right)

    def ag_start(k):
        for q in range(PARTS):
            for way in range(2):
                ag_copy(way, k, q).start()

    def ag_next(k):
        for q in range(PARTS):
            for way in range(2):
                ag_got(way, k, q).wait_recv()
                if k < half_z:
                    ag_copy(way, k + 1, q).start()

    def role(r):
        s = mod(x - z - r, n_x)
        return s, s * quads + zq < tiles

    x_to = {0: {"tp": mod(x + 1, n_x)}, 1: {"tp": mod(x - 1, n_x)}}
    fours = n_z // 4

    def group(core, s, g):
        return w.at[s, core, pl.ds(g * fours, fours)]

    def xf_copy(g, way, s):
        return remote(group(c, s, g), xf_send.at[g, way], xf_recv.at[g, way], x_to[way])

    def xh_copy(g, s):
        return remote(group(c, s, g), xh_send.at[g], xh_recv.at[g], x_to[g // 2])

    def p_copy(g, r, s):
        return remote(group(c, s, g), p_send.at[g, r], p_recv.at[g, r], other)

    def x_owner(g):
        s, valid = role(0)

        @pl.when(valid)
        def _():
            for chip in range(g * fours, (g + 1) * fours):

                @pl.when(z != chip)
                def _(chip=chip):
                    remote(w.at[s, c, chip], st_sent.at[chip], st_recv.at[chip], right).wait_recv()

            for way in range(2):
                xf_copy(g, way, s).start()
            p_copy(g, 0, s).start()

    def x_relay(g):
        for way, r in ((0, 1), (1, 3)):
            s, valid = role(r)

            @pl.when(valid)
            def _(way=way, r=r, s=s):
                xf_copy(g, way, s).wait_recv()
                if g // 2 == way:
                    xh_copy(g, s).start()
                p_copy(g, r, s).start()

    def x_last(g):
        s, valid = role(2)

        @pl.when(valid)
        def _():
            xh_copy(g, s).wait_recv()
            p_copy(g, 2, s).start()

    def x_partner(g):
        for r in range(4):
            s, valid = role(r)

            @pl.when(valid)
            def _(r=r, s=s):
                remote(group(1 - c, s, g), p_send.at[g, r], p_recv.at[g, r], other).wait_recv()

    ag_start(1)
    after = {
        0: [(x_owner, 0), (x_owner, 1)],
        1: [(x_owner, 2)],
        2: [(x_owner, 3)],
        3: [(x_relay, 0)],
        4: [(x_relay, 1)],
        5: [(x_relay, 2), (x_last, 0)],
        6: [(x_relay, 3), (x_last, 1)],
        7: [(x_last, 2)],
        8: [(x_last, 3)] + [(x_partner, g) for g in range(4)],
    }
    for k in range(half_z + 1):
        if k:
            ag_next(k)
        for what, g in after.get(k, ()):
            what(g)

    rbuf[0, 0, half_rows:, :] = jnp.zeros((own_rows - half_rows, d), BF)
    rbuf[1, 0, 0:half_rows, :] = jnp.zeros((half_rows, d), BF)

    def rs_copy(way, i, q, whole):
        rows = pl.ds(0, own_rows) if whole else pl.ds(way * half_rows, half_rows)
        lanes = pl.ds(q * wide_part, wide_part)
        return pltpu.make_async_remote_copy(
            src_ref=sbuf.at[way, i, rows, lanes], dst_ref=rbuf.at[way, i, rows, lanes],
            send_sem=rs_send.at[way, i, q], recv_sem=rs_recv.at[way, i, q],
            device_id=right if way == 0 else left, device_id_type=MESH,
        )

    def matrix(core, kinds):
        at = [(m * d_block, s) for m in kinds for s in range(slots)]
        return jnp.concatenate([w[s, core, :, r : r + d_block, :].reshape(d_half, LANES) for r, s in at], axis=1)

    def ring_step(i, unused):
        far = half_z - i
        one_at = mod(z + far, n_z)
        two_at = jnp.where(i == 0, z, mod(z - far, n_z))
        rows2 = jnp.concatenate([act[one_at], act[two_at]], axis=0)
        sums = dot(rows2[:, 0:d_half], matrix(0, (0, 1))) + dot(rows2[:, d_half:], matrix(1, (0, 1)))
        gate, up = sums[:, 0:ff_pad], sums[:, ff_pad:]
        hidden = (gate / (1.0 + jnp.exp(-gate)) * up).astype(BF)
        part[:, 0:d_half] = dot_t(hidden, matrix(0, (2,)))
        part[:, d_half:] = dot_t(hidden, matrix(1, (2,)))

        @pl.when(i == 0)
        def _():
            own[...] = part[own_rows:, :]
            far_sum = part[0:own_rows, :].astype(BF)
            for way in range(2):
                sbuf[way, 0] = far_sum
            for q in range(PARTS):
                for way in range(2):
                    rs_copy(way, 0, q, False).start()

        def pass_on(i, whole):
            for q in range(PARTS):
                lanes = slice(q * wide_part, (q + 1) * wide_part)
                for way in range(2):
                    rs_copy(way, i - 1, q, whole).wait_recv()
                    mine = part[way * own_rows : (way + 1) * own_rows, lanes]
                    sbuf[way, i, :, lanes] = (rbuf[way, i - 1, :, lanes].astype(F32) + mine).astype(BF)
                    rs_copy(way, i, q, True).start()

        @pl.when(i == 1)
        def _():
            pass_on(1, False)

        @pl.when(i > 1)
        def _():
            pass_on(i, True)

        return unused

    lax.fori_loop(0, half_z, ring_step, 0)
    for way in range(2):
        for q in range(PARTS):
            rs_copy(way, half_z - 1, q, True).wait_recv()
    total = own[...] + rbuf[0, half_z - 1].astype(F32) + rbuf[1, half_z - 1].astype(F32)
    out_ref[...] = (stream[...] + swap_halves(total, False)).astype(out_ref.dtype)

    e_copy.wait_send()

    def g_sent(to, unused):
        g_copy(to).wait_send()
        return unused

    lax.fori_loop(z + 1, n_z, g_sent, 0)

    def st_left(k, unused):
        chip = st_chip(k)
        s, j = tile_of(chip)

        @pl.when(j < tiles)
        def _():
            st_copy(chip, s, j).wait_send()

        return unused

    lax.fori_loop(0, n_z - 1, st_left, 0)
    for k in range(1, n_x):
        m_copy(k).wait_send()
    for way in range(2):
        for k in range(1, half_z + 1):
            for q in range(PARTS):
                ag_copy(way, k, q).wait_send()
        for i in range(half_z):
            for q in range(PARTS):
                rs_copy(way, i, q, i > 0).wait_send()
    for g in range(4):
        for r in range(4):
            s, valid = role(r)

            @pl.when(valid)
            def _(g=g, r=r, s=s):
                p_copy(g, r, s).wait_send()
                if r == 0:
                    xf_copy(g, 0, s).wait_send()
                    xf_copy(g, 1, s).wait_send()
                if (r, g // 2) in ((1, 0), (3, 1)):
                    xh_copy(g, s).wait_send()


def per_device(
    ssm_input, residual_in, log_step, decay_real, freq, in_real, in_imag, out_real, out_imag, skip,
    w_glu, b_glu, w_branch, norm_gain, w_gate, w_up, w_down,
):
    tok, width = ssm_input.shape
    groups, n_p = decay_real.shape
    group_size = in_real.shape[2]
    n_z, n_c, n_x = lax.axis_size("sp_0"), lax.axis_size("sp_1"), lax.axis_size("tp")
    d = residual_in.shape[1]
    wide = w_glu.shape[0]
    tiles = w_gate.shape[1] // LANES
    quads = n_z // n_x
    slots = -(-tiles // quads)
    assert n_c == 2 and n_x == 4 and slots < n_x and n_z % n_x == 0
    assert tok == SPAN * ROWS8 and 2 * n_p == LANES and w_gate.shape[1] % LANES == 0
    own_rows = tok // n_x
    n_state = groups * n_p
    half_z = n_z // 2
    vmem = pl.BlockSpec(memory_space=pltpu.VMEM)
    hbm = pl.BlockSpec(memory_space=pl.ANY)
    dma = pltpu.SemaphoreType.DMA
    return pl.pallas_call(
        functools.partial(kernel, (n_z, n_x, tiles, slots)),
        out_shape=jax.ShapeDtypeStruct((own_rows, d), BF),
        in_specs=[vmem] * 11 + [hbm] * 6,
        out_specs=vmem,
        scratch_shapes=[
            pltpu.VMEM((wide, wide), BF),
            pltpu.VMEM((wide, d), BF),
            pltpu.VMEM((own_rows, d), BF),
            pltpu.VMEM((tiles, 3 * w_gate.shape[0], LANES), BF),
            pltpu.VMEM((slots, 2, n_z, 3 * w_gate.shape[0], LANES), BF),
            pltpu.VMEM((width, 2 * n_state), BF),
            pltpu.VMEM((width, 2 * n_state), BF),
            pltpu.VMEM((tok, 2 * n_state), F32),
            pltpu.VMEM((tok, 2 * n_state), BF),
            pltpu.VMEM((3, 2, n_state), F32),
            pltpu.VMEM((n_z, 2, n_state), F32),
            pltpu.VMEM((n_x, own_rows, width), BF),
            pltpu.VMEM((n_x, own_rows, width), BF),
            pltpu.VMEM((n_z, own_rows, d), BF),
            pltpu.VMEM((own_rows, d), F32),
            pltpu.VMEM((own_rows, d), F32),
            pltpu.VMEM((2 * own_rows, d), F32),
            pltpu.VMEM((2, half_z, own_rows, d), BF),
            pltpu.VMEM((2, half_z, own_rows, d), BF),
            dma((3,)), dma((n_z,)), dma((n_z,)), dma((1,)), dma((1,)), dma((n_z,)), dma((n_z,)),
            dma((n_x,)), dma((n_x,)),
            dma((4, 2)), dma((4, 2)), dma((4,)), dma((4,)), dma((4, 4)), dma((4, 4)),
            dma((2, half_z, PARTS)), dma((2, half_z, PARTS)), dma((2, half_z, PARTS)), dma((2, half_z, PARTS)),
            dma((3, tiles)),
        ],
        compiler_params=pltpu.CompilerParams(collective_id=0, has_side_effects=True, vmem_limit_bytes=56 * 1024 * 1024),
        name="mixer_ffn",
    )(
        ssm_input,
        log_step.reshape(1, groups),
        decay_real,
        freq,
        in_real.transpose(0, 2, 1).reshape(groups * group_size, n_p),
        in_imag.transpose(0, 2, 1).reshape(groups * group_size, n_p),
        out_real.reshape(groups * group_size, n_p),
        out_imag.reshape(groups * group_size, n_p),
        skip.reshape(1, width),
        b_glu.reshape(1, wide),
        norm_gain.reshape(1, d),
        residual_in,
        w_glu,
        w_branch,
        w_gate,
        w_up,
        w_down.T,
    )


def solution(mesh):
    n_c = 2
    torus = Mesh(
        mesh.devices.reshape(mesh.shape["grp"], mesh.shape["sp"] // n_c, n_c, mesh.shape["tp"]),
        ("grp", "sp_0", "sp_1", "tp"),
    )
    in_specs = (
        P(GRP_SP, "tp"), P(GRP_SP, None), P("tp"), P("tp", None), P("tp", None),
        P("tp", None, None), P("tp", None, None), P("tp", None, None), P("tp", None, None), P("tp"),
        P(), P(), P(), P(), P(SP, "tp"), P(SP, "tp"), P("tp", SP),
    )
    return jax.shard_map(per_device, mesh=torus, in_specs=in_specs, out_specs=P(GRP_SP_TP, None), check_vma=False)
```
